32 devices in a mesh: sp: 4 (over y, x), tp: 8 (over z, core).
Axes of the slice: x: 2, y: 2, z: 4, core: 2. Of those that a mesh axis runs over, the one named last changes fastest.
Arguments:
- receptance: bfloat16 [1024, 1024], P('sp', 'tp'), may hold values from -6 to 6
- key_matrix: bfloat16 [1024, 1024], P('sp', 'tp'), may hold values from -6 to 6
- value_matrix: bfloat16 [1024, 1024], P('sp', 'tp'), may hold values from -6 to 6
- decay_input_term: bfloat16 [1024, 1024], P('sp', 'tp'), may hold values from -5 to 5
- decay_channel_offset: float32 [1024], P('tp'), may hold values from -12 to -2
- head_log_decay: float32 [1024, 16], P('sp', 'tp'), may hold values from -2 to 0
- context_step_logits: bfloat16 [1024, 1024], P('sp', 'tp'), may hold values from -16 to 4
- head_gate_rows: bfloat16 [1024, 1024], P('sp', 'tp'), may hold values from -6 to 6
- head_norm_scale: float32 [1024], P('tp'), may hold values from 0.1 to 1.9
- mixer_output_weight: bfloat16 [1024, 2048], replicated, may hold values from -0.1875 to 0.1875
- residual: bfloat16 [1024, 2048], P(('sp', 'tp')), may hold values from -6 to 6
- expert_norm_scale: float32 [2048], replicated, may hold values from 0.1 to 1.9
- expert_index_table: int32 [1024, 2], P(('sp', 'tp')), may hold values from 0 to 3, all different within a row; in each aligned block of 32 rows (0 to 31, 32 to 63, ...) at most 32 rows name the same one
- expert_router_scores: float32 [1024, 2], P(('sp', 'tp')), may hold values from -6 to 6
- expert_gate_weight: bfloat16 [4, 2048, 7168], P('sp', None, 'tp'), may hold values from -0.125 to 0.125
- expert_up_weight: bfloat16 [4, 2048, 7168], P('sp', None, 'tp'), may hold values from -0.125 to 0.125
- expert_down_weight: bfloat16 [4, 7168, 2048], P('sp', 'tp'), may hold values from -0.0625 to 0.0625
Outputs:
- layer_out: bfloat16 [1024, 2048], P(('sp', 'tp'))
The draws below stay inside these ranges and needn't reach their ends.
Inputs may be any that keep to these rules, and one draw needn't show every extreme that they name: `expert_index_table`: each row names 2 different experts. In each aligned block of 32 rows no expert is named more than 32 times, a bound that some block reaches.
All inputs are finite; a program needn't handle non-finite values.
Results may differ from the reference program's by a relative error of at most 0.018.
Values may be sent and summed in bfloat16 or wider, within the bound.
A program may use at most 64 MiB of HBM per device.

```python
import math
import jax
import jax.numpy as jnp
import numpy as np
from jax import lax

D = 2048
HEADS = 16
HEAD_CHANNELS = 64
FF = 7168
TOPK = 2
WIDTH = 1024
TOKENS = 1024
EXPERTS = 4
ROWS = 32
CAP = 32
N_TP = 8


def head_kinds(key):
    order = jax.random.permutation(jax.random.fold_in(key, 101), HEADS)
    slow = order < HEADS // 2
    return jnp.repeat(slow, HEAD_CHANNELS)


def noise(key, array_shape):
    return jnp.clip(jax.random.normal(key, array_shape, jnp.float32), -4.0, 4.0)


def draw_decay_channel_offset(key, part):
    slow = head_kinds(key)
    fast_level = jnp.repeat(jax.random.uniform(jax.random.fold_in(key, 102), (HEADS,), jnp.float32, -3.5, -3.0), HEAD_CHANNELS)
    jitter = jax.random.uniform(jax.random.fold_in(key, 103), (WIDTH,), jnp.float32, -0.5, 0.5)
    slow_level = math.log(0.17 / TOKENS)
    return jnp.where(slow, slow_level, fast_level) + jitter


def draw_context_step_logits(key, part):
    slow = head_kinds(key)
    level = jnp.where(slow, math.log(0.5 * HEAD_CHANNELS / TOKENS), 0.0)
    shifted = noise(jax.random.fold_in(key, 104), (TOKENS, WIDTH)) + level[None, :]
    return shifted.astype(jnp.bfloat16)


def draw_decay_input_term(key, part):
    offset = jax.random.uniform(jax.random.fold_in(key, 105), (TOKENS // 128, 1, 1), jnp.float32, -1.0, 1.0)
    shifted = noise(jax.random.fold_in(key, 106), (TOKENS // 128, 128, WIDTH)) + offset
    return shifted.reshape(TOKENS, WIDTH).astype(jnp.bfloat16)


def draw_head_log_decay(key, part):
    where_at = jax.random.randint(jax.random.fold_in(key, 107), (2,), 0, TOKENS)
    strength = jax.random.uniform(jax.random.fold_in(key, 108), (2, HEADS), jnp.float32, math.log(0.5), math.log(0.8))
    position = jnp.arange(TOKENS, dtype=jnp.int32)
    marked = (position[:, None, None] == where_at[None, :, None]).astype(jnp.float32)
    return jnp.sum(marked * strength[None, :, :], axis=1)


def level_of(own_key, dims, shards, smallest, high):
    def one(axis_at, shards_of):
        steps = jax.random.uniform(jax.random.fold_in(jax.random.fold_in(own_key, 6), axis_at), (shards_of,), jnp.float32, smallest / len(shards), high / len(shards))
        return jnp.repeat(jnp.exp(steps), dims[axis_at] // shards_of).reshape((-1,) + (1,) * (len(dims) - axis_at - 1))

    factor_of = one(*shards[0])
    for cut in shards[1:]:
        factor_of = factor_of * one(*cut)
    return factor_of


def shared_out(own_key, own, number, rows, amount, top, reach, skew):
    sequence = jax.random.permutation(own_key, amount)
    heavy_load, usual = portions_of(amount, rows * top, reach, skew, True), portions_of(amount, rows * top, reach, skew, False)
    places = jnp.arange(amount)

    def named(lengths, turn):
        used = int((lengths > 0).sum())
        fixed = max(1, used // 4)
        moved = fixed + (places - fixed + turn * (used - fixed)) % max(1, amount - fixed)
        return jnp.zeros((amount,), jnp.int32).at[sequence[jnp.where(places < fixed, places, moved)]].set(jnp.asarray(lengths, jnp.int32))

    lengths = jnp.where(number % 4 == 0, named(heavy_load, number // 4), named(usual, number - number // 4 - 1))
    mixed = jax.random.permutation(jax.random.fold_in(own, 3), amount)
    source_of, taker = mixed[0:amount // 2 * 2:2], mixed[1:amount // 2 * 2:2]
    margin = jnp.minimum(lengths[source_of] - 1, reach - lengths[taker]) // 2
    margin = jnp.where((source_of == sequence[0]) | (taker == sequence[0]) | (lengths[taker] == 0), 0, jnp.maximum(margin, 0))
    moved = jax.random.randint(jax.random.fold_in(own, 4), (amount // 2,), 0, 1 << 20) % (margin + 1)
    lengths = lengths.at[source_of].add(-moved).at[taker].add(moved)
    items = jnp.searchsorted(jnp.cumsum(lengths), jnp.arange(rows * top), side="right").astype(jnp.int32)
    table = items.reshape(top, rows).T
    table = table[jax.random.permutation(jax.random.fold_in(own, 1), rows)]
    turn = jax.random.randint(jax.random.fold_in(own, 2), (rows, 1), 0, top)
    return jnp.take_along_axis(table, (jnp.arange(top)[None, :] + turn) % top, axis=1)


def portions_of(number_of, total, most, skew, full):
    weights = [(1 << 20) // math.isqrt(standing ** skew) + 1 for standing in range(1, number_of + 1)]
    largest = most if full else min(most, max(-(-total // number_of), total * weights[0] // sum(weights)))
    least = 1 if total - largest >= number_of - 1 else 0
    counts, rest = [largest] + [least] * (number_of - 1), total - largest - least * (number_of - 1)
    while rest > 0:
        candidates = [i for i in range(1, number_of) if counts[i] < largest] or [i for i in range(1, number_of) if counts[i] < most]
        whole, budget = sum([weights[i] for i in candidates]), rest
        for i in candidates:
            extra = min(most - counts[i], max(1, budget * weights[i] // whole), rest)
            counts[i] = counts[i] + extra
            rest = rest - extra
    return np.array(counts)


def normal_values(stream_key, extent, scale, limit, pieces=(), kind=jnp.bfloat16):
    drawn = jax.random.normal(stream_key, extent, jnp.float32) * scale
    if len(pieces) > 0:
        drawn = level_of(stream_key, extent, pieces, -0.22, 0.18) * drawn
    return jnp.clip(drawn, min=-limit, max=limit).astype(kind)


def setup_inputs(seed: int = 0) -> dict:
    keys = jax.random.split(jax.random.key(seed), 18)
    receptance = normal_values(keys[0], (TOKENS, WIDTH), 1.0, 6.0, ((0, 4), (1, 8)))
    key_matrix = normal_values(keys[1], (TOKENS, WIDTH), 1.0, 6.0, ((0, 4), (1, 8)))
    value_matrix = normal_values(keys[2], (TOKENS, WIDTH), 1.0, 6.0, ((0, 4), (1, 8)))
    decay_input_term = draw_decay_input_term(jax.random.fold_in(keys[17], 71), 0)
    decay_channel_offset = draw_decay_channel_offset(jax.random.fold_in(keys[17], 71), 0)
    head_log_decay = draw_head_log_decay(jax.random.fold_in(keys[17], 71), 0)
    context_step_logits = draw_context_step_logits(jax.random.fold_in(keys[17], 71), 0)
    head_gate_rows = normal_values(keys[7], (TOKENS, WIDTH), 1.0, 6.0, ((0, 4), (1, 8)))
    head_norm_scale = jnp.clip(1.0 + 0.18 * jax.random.normal(keys[8], (WIDTH,), jnp.float32), 0.1, 1.9)
    mixer_output_weight = normal_values(keys[9], (WIDTH, D), WIDTH ** -0.5, 0.1875)
    residual = normal_values(keys[10], (TOKENS, D), 1.0, 6.0, ((0, 32),))
    expert_norm_scale = jnp.clip(1.0 + 0.18 * jax.random.normal(keys[11], (D,), jnp.float32), 0.1, 1.9)
    expert_index_table_keys = jax.random.split(jax.random.fold_in(keys[12], 1), TOKENS // ROWS)
    expert_index_table_turns = jax.random.permutation(jax.random.fold_in(keys[12], 3), TOKENS // ROWS)
    expert_index_table = jax.vmap(lambda own, number: shared_out(jax.random.fold_in(keys[12], 2), own, number, ROWS, EXPERTS, TOPK, CAP, 1))(expert_index_table_keys, expert_index_table_turns).reshape((TOKENS, TOPK))
    expert_router_scores = normal_values(keys[13], (TOKENS, TOPK), 1.5, 6.0, ((0, 32),), jnp.float32)
    expert_gate_weight = normal_values(keys[14], (EXPERTS, D, FF), D ** -0.5, 0.125, ((0, 4), (2, 8)))
    expert_up_weight = normal_values(keys[15], (EXPERTS, D, FF), D ** -0.5, 0.125, ((0, 4), (2, 8)))
    expert_down_weight = normal_values(keys[16], (EXPERTS, FF, D), FF ** -0.5, 0.0625, ((0, 4), (1, 8)))
    return {"receptance": receptance, "key_matrix": key_matrix, "value_matrix": value_matrix, "decay_input_term": decay_input_term, "decay_channel_offset": decay_channel_offset, "head_log_decay": head_log_decay, "context_step_logits": context_step_logits, "head_gate_rows": head_gate_rows, "head_norm_scale": head_norm_scale, "mixer_output_weight": mixer_output_weight, "residual": residual, "expert_norm_scale": expert_norm_scale, "expert_index_table": expert_index_table, "expert_router_scores": expert_router_scores, "expert_gate_weight": expert_gate_weight, "expert_up_weight": expert_up_weight, "expert_down_weight": expert_down_weight}


decay_factor = 0.6065306597126334
group_eps = 0.00064
norm_eps = 1e-06
key_eps = 1e-06
highest = lax.Precision.HIGHEST

def per_head_input(receptance, key_matrix, value_matrix, decay_input_term, decay_channel_offset, head_log_decay, context_step_logits):
    head_split_shape = (receptance.shape[0], head_log_decay.shape[1], HEAD_CHANNELS)
    read_vec = receptance.astype(jnp.float32).reshape(head_split_shape)
    key_vec = key_matrix.astype(jnp.float32).reshape(head_split_shape)
    value_vec = value_matrix.astype(jnp.float32).reshape(head_split_shape)
    decay_logits = (decay_input_term.astype(jnp.float32) + decay_channel_offset[None, :]).reshape(head_split_shape)
    decay_vector = jnp.exp(-decay_factor * jax.nn.sigmoid(decay_logits) + head_log_decay[:, :, None])
    learn_vec = jax.nn.sigmoid(context_step_logits.astype(jnp.float32)).reshape(head_split_shape)
    unit_vec = key_vec * lax.rsqrt(lax.optimization_barrier(jnp.sum(key_vec * key_vec, axis=-1, keepdims=True)) + key_eps)
    return (read_vec, decay_vector, -unit_vec, unit_vec * learn_vec, key_vec * learn_vec, value_vec)

def finish(mixer_out, head_norm_scale, head_gate_rows):
    average = lax.optimization_barrier(jnp.mean(mixer_out, axis=-1, keepdims=True))
    centred = mixer_out - average
    spread = lax.optimization_barrier(jnp.mean(centred * centred, axis=-1, keepdims=True))
    normed = (centred * lax.rsqrt(spread + group_eps)).reshape(mixer_out.shape[0], -1)
    return (normed * head_norm_scale[None, :] * head_gate_rows.astype(jnp.float32)).astype(jnp.bfloat16)

def advance(state_mat, packed):
    read_vec, decay_vector, erase_vec, write_vec, keyed_vec, value_vec = packed
    recall = jnp.einsum('hvk,hk->hv', state_mat, erase_vec, precision=highest)
    state_mat = state_mat * decay_vector[:, None, :] + recall[:, :, None] * write_vec[:, None, :] + value_vec[:, :, None] * keyed_vec[:, None, :]
    return (state_mat, jnp.einsum('hvk,hk->hv', state_mat, read_vec, precision=highest))

def expert_outputs(normed, expert_index_table, expert_gate_weight, expert_up_weight, expert_down_weight):
    block_count = TOKENS // ROWS
    chosen = expert_index_table.reshape(block_count, ROWS * TOPK)
    matches = (chosen[:, :, None] == jnp.arange(EXPERTS, dtype=jnp.int32)[None, None, :]).astype(jnp.int32)
    slot_of = lax.optimization_barrier(jnp.sum(jnp.cumsum(matches, axis=1) * matches, axis=2)) - 1
    block_of = jnp.arange(block_count, dtype=jnp.int32)[:, None]
    placing = (chosen * (block_count * CAP) + block_of * CAP + slot_of).astype(jnp.int32)
    token_of = (block_of * ROWS + jnp.arange(ROWS * TOPK, dtype=jnp.int32)[None, :] // TOPK).astype(jnp.int32)
    routing = jnp.full((EXPERTS * block_count * CAP,), TOKENS, jnp.int32).at[placing.reshape(-1)].set(token_of.reshape(-1))
    padded = jnp.concatenate([normed, jnp.zeros((1, D), jnp.bfloat16)], axis=0)
    block_width = FF // N_TP

    def one_expert(packed):
        slot_index, gate_mat, up_mat, down_mat = packed
        picked = padded[slot_index]
        gate_act = jnp.dot(picked, gate_mat, preferred_element_type=jnp.float32)
        up_act = jnp.dot(picked, up_mat, preferred_element_type=jnp.float32)
        hidden = (jax.nn.silu(gate_act) * up_act).astype(jnp.bfloat16)
        partials = jnp.einsum('rjf,jfd->jrd', hidden.reshape(-1, N_TP, block_width).astype(jnp.float32), down_mat.reshape(N_TP, block_width, D).astype(jnp.float32))
        rounded = lax.optimization_barrier(partials.astype(jnp.bfloat16))
        return lax.optimization_barrier(jnp.sum(rounded.astype(jnp.float32), axis=0)).astype(jnp.bfloat16)
    results = lax.map(one_expert, (routing.reshape(EXPERTS, -1), expert_gate_weight, expert_up_weight, expert_down_weight))
    flat_out = results.reshape(-1, D)
    return flat_out[placing.reshape(-1)].reshape(TOKENS, TOPK, D)

def reference(receptance, key_matrix, value_matrix, decay_input_term, decay_channel_offset, head_log_decay, context_step_logits, head_gate_rows, head_norm_scale, mixer_output_weight, residual, expert_norm_scale, expert_index_table, expert_router_scores, expert_gate_weight, expert_up_weight, expert_down_weight):
    input_rows = per_head_input(receptance, key_matrix, value_matrix, decay_input_term, decay_channel_offset, head_log_decay, context_step_logits)
    state_zero = jnp.zeros((HEADS, HEAD_CHANNELS, HEAD_CHANNELS), jnp.float32)
    _, mixer_out = lax.scan(advance, state_zero, input_rows)
    attended = finish(mixer_out, head_norm_scale, head_gate_rows)
    mixed = (residual.astype(jnp.float32) + jnp.dot(attended, mixer_output_weight, preferred_element_type=jnp.float32)).astype(jnp.bfloat16)
    mixed_f = mixed.astype(jnp.float32)
    normed = (mixed_f * lax.rsqrt(lax.optimization_barrier(jnp.mean(mixed_f * mixed_f, axis=-1, keepdims=True)) + norm_eps) * expert_norm_scale[None, :]).astype(jnp.bfloat16)
    pair_out = expert_outputs(normed, expert_index_table, expert_gate_weight, expert_up_weight, expert_down_weight)
    weights = jax.nn.sigmoid(expert_router_scores - expert_router_scores[:, ::-1])
    total = mixed_f + lax.optimization_barrier(jnp.sum(weights[:, :, None] * pair_out.astype(jnp.float32), axis=1))
    return total.astype(jnp.bfloat16)
```

```python
import jax
import jax.numpy as jnp
from jax import lax
from jax.experimental import pallas as pl
from jax.experimental.pallas import tpu as pltpu
from jax.sharding import PartitionSpec as P

TOPK = 2


decay_factor = 0.6065306597126334
group_eps = 0.00064
norm_eps = 1e-06
key_eps = 1e-06
highest = lax.Precision.HIGHEST
block_len = 64


def dot(left, right, dims=((1,), (0,))):
    return lax.dot_general(
        left, right, (dims, ((), ())), precision=highest, preferred_element_type=jnp.float32
    )


def mixer_kernel(
    read_ref, key_ref, value_ref, decay_ref, offset_ref, log_ref, step_ref, out_ref, final_ref
):
    tokens, width = read_ref.shape
    heads = log_ref.shape[1]
    chan = width // heads
    block = block_len
    count = tokens // block
    row = lax.broadcasted_iota(jnp.int32, (tokens, tokens), 0)
    col = lax.broadcasted_iota(jnp.int32, (tokens, tokens), 1)

    def same(size):
        shift = size.bit_length() - 1
        return (row >> shift) == (col >> shift)

    lower = jnp.logical_and(same(block), col <= row)
    read = read_ref[...].astype(jnp.float32)
    key = key_ref[...].astype(jnp.float32)
    value = value_ref[...].astype(jnp.float32)
    learn = jax.nn.sigmoid(step_ref[...].astype(jnp.float32))
    logs = jnp.concatenate(
        [jnp.broadcast_to(log_ref[:, h : h + 1], (tokens, chan)) for h in range(heads)], axis=1
    )
    logs = logs - decay_factor * jax.nn.sigmoid(decay_ref[...].astype(jnp.float32) + offset_ref[...])
    total = dot(jnp.where(lower, 1.0, 0.0), logs)
    blocked = total.reshape(count, block, width)
    centre = jnp.broadcast_to(blocked[:, block // 2 - 1 : block // 2], blocked.shape)
    centre = centre.reshape(tokens, width)
    last = blocked[:, block - 1 : block]
    ending = jnp.broadcast_to(last, blocked.shape).reshape(tokens, width)
    squares = key * key
    norm = jnp.concatenate(
        [
            jnp.broadcast_to(
                jnp.sum(squares[:, h * chan : (h + 1) * chan], axis=1, keepdims=True), (tokens, chan)
            )
            for h in range(heads)
        ],
        axis=1,
    )
    unit = key * lax.rsqrt(norm + key_eps)
    write = unit * learn
    keyed = key * learn
    before = total - logs
    fade = jnp.exp(total - centre)
    grow = jnp.exp(centre - total)
    erase_mid = -unit * jnp.exp(before - centre)
    read_mid = read * fade
    write_mid = write * grow
    keyed_mid = keyed * grow
    erase_in = -unit * jnp.exp(before)
    read_in = read * jnp.exp(total)
    leave = jnp.exp(ending - total)
    write_out = write * leave
    keyed_out = keyed * leave
    through = jnp.exp(last.reshape(count, width))
    eye_row = lax.broadcasted_iota(jnp.int32, (chan, chan), 0)
    eye_col = lax.broadcasted_iota(jnp.int32, (chan, chan), 1)
    for h in range(heads):
        at = slice(h * chan, (h + 1) * chan)
        gram = dot(
            jnp.concatenate([erase_mid[:, at], read_mid[:, at]], axis=0),
            jnp.concatenate([write_mid[:, at], keyed_mid[:, at]], axis=0),
            ((1,), (1,)),
        )
        erase_write = gram[:tokens, :tokens]
        strict = jnp.logical_and(same(block), col < row)
        erase_keyed = jnp.where(strict, gram[:tokens, tokens:], 0.0)
        read_write = jnp.where(lower, gram[tokens:, :tokens], 0.0)
        read_keyed = jnp.where(lower, gram[tokens:, tokens:], 0.0)
        inverse = jnp.where(row == col, 1.0, 0.0)
        size = 1
        while size < block:
            pair = jnp.logical_and(same(2 * size), jnp.logical_and(~same(size), col < row))
            part = jnp.where(pair, erase_write, 0.0)
            if size == 1:
                inverse = inverse + part
            else:
                inverse = inverse + dot(inverse, dot(part, inverse))
            size *= 2
        seen = dot(erase_keyed, value[:, at])
        solved = dot(inverse, jnp.concatenate([seen, erase_in[:, at]], axis=1))
        given = jnp.concatenate([value[:, at], jnp.zeros((tokens, chan), jnp.float32)], axis=1)
        local = dot(read_write, solved) + dot(read_keyed, given)
        mapped = local[:, chan:] + read_in[:, at]
        state = jnp.concatenate(
            [jnp.zeros((chan, chan), jnp.float32), jnp.where(eye_row == eye_col, 1.0, 0.0)], axis=1
        )
        for c in range(count):
            rows = slice(c * block, (c + 1) * block)
            out = dot(mapped[rows], state)
            out_ref[h, rows, :] = out + jnp.concatenate(
                [local[rows, :chan], jnp.zeros((block, chan), jnp.float32)], axis=1
            )
            step = dot(write_out[rows, at], solved[rows], ((0,), (0,)))
            step = step + dot(keyed_out[rows, at], given[rows], ((0,), (0,)))
            shift_map = step[:, chan:] + jnp.where(eye_row == eye_col, through[c : c + 1, at], 0.0)
            state = dot(shift_map, state) + jnp.concatenate(
                [step[:, :chan], jnp.zeros((chan, chan), jnp.float32)], axis=1
            )
        final_ref[h] = state.astype(final_ref.dtype)


def finish_kernel(gathered_ref, out_ref, scale_ref, gate_ref, attended_ref):
    laps, heads, chan, _ = gathered_ref.shape
    place = lax.axis_index("sp")

    def one(lap, states):
        joined = []
        for h in range(heads):
            later = gathered_ref[lap, h].astype(jnp.float32)
            after = dot(later[:, chan:], states[h]) + later[:, :chan]
            joined.append(jnp.where(lap < place, after, states[h]))
        return tuple(joined)

    start = tuple(jnp.zeros((chan, chan), jnp.float32) for _ in range(heads))
    states = lax.fori_loop(0, laps - 1, one, start)
    pieces = []
    for h in range(heads):
        out = out_ref[h]
        mixer_out = out[:, :chan] + dot(out[:, chan:], states[h])
        centred = mixer_out - jnp.mean(mixer_out, axis=-1, keepdims=True)
        spread = jnp.mean(centred * centred, axis=-1, keepdims=True)
        pieces.append(centred * lax.rsqrt(spread + group_eps))
    normed = jnp.concatenate(pieces, axis=1)
    attended_ref[...] = (normed * scale_ref[...] * gate_ref[...].astype(jnp.float32)).astype(
        attended_ref.dtype
    )


def dispatch_tables(chosen, experts, capacity):
    row_count = chosen.shape[0]
    flat_ids = chosen.reshape(-1)
    matches = (flat_ids[:, None] == jnp.arange(experts, dtype=jnp.int32)[None, :]).astype(jnp.int32)
    slot_of = jnp.sum(jnp.cumsum(matches, axis=0) * matches, axis=1) - 1
    placing = flat_ids * capacity + slot_of
    routing = jnp.arange(experts * capacity, dtype=jnp.int32)[:, None] == placing[None, :]
    spread_rows = jnp.any(routing.reshape(experts * capacity, row_count, chosen.shape[1]), axis=2)
    return (spread_rows.astype(jnp.bfloat16), routing.astype(jnp.bfloat16))


def expand(rows_in, gate_mat, up_mat):
    gate_act = jnp.dot(rows_in, gate_mat, preferred_element_type=jnp.float32)
    up_act = jnp.dot(rows_in, up_mat, preferred_element_type=jnp.float32)
    return (jax.nn.silu(gate_act) * up_act).astype(jnp.bfloat16)


def shards(
    receptance,
    key_matrix,
    value_matrix,
    decay_input_term,
    decay_channel_offset,
    head_log_decay,
    context_step_logits,
    head_gate_rows,
    head_norm_scale,
    mixer_output_weight,
    residual,
    expert_norm_scale,
    expert_index_table,
    expert_router_scores,
    expert_gate_weight,
    expert_up_weight,
    expert_down_weight,
):
    tokens, width = receptance.shape
    heads = head_log_decay.shape[1]
    chan = width // heads
    local, final = pl.pallas_call(
        mixer_kernel,
        out_shape=(
            jax.ShapeDtypeStruct((heads, tokens, 2 * chan), jnp.float32),
            jax.ShapeDtypeStruct((heads, chan, 2 * chan), jnp.bfloat16),
        ),
    )(
        receptance,
        key_matrix,
        value_matrix,
        decay_input_term,
        decay_channel_offset[None, :],
        head_log_decay,
        context_step_logits,
    )
    gathered = lax.all_gather(final, "sp")
    attended = pl.pallas_call(
        finish_kernel, out_shape=jax.ShapeDtypeStruct((tokens, width), jnp.bfloat16)
    )(gathered, local, head_norm_scale[None, :], head_gate_rows)
    row_count = residual.shape[0]
    token_rows = lax.all_to_all(attended, "tp", split_axis=0, concat_axis=1, tiled=True)
    projected = jnp.dot(token_rows, mixer_output_weight, preferred_element_type=jnp.float32)
    mixed = (residual.astype(jnp.float32) + projected).astype(jnp.bfloat16)
    mixed_f = mixed.astype(jnp.float32)
    normed = (
        mixed_f
        * lax.rsqrt(jnp.mean(mixed_f * mixed_f, axis=-1, keepdims=True) + norm_eps)
        * expert_norm_scale[None, :]
    ).astype(jnp.bfloat16)
    model_width = normed.shape[1]
    sp_size = lax.axis_size("sp")
    experts = sp_size * expert_gate_weight.shape[0]
    capacity = 2 * row_count * TOPK // experts
    gate_mat, up_mat, down_mat = (expert_gate_weight[0], expert_up_weight[0], expert_down_weight[0])
    spread_own, routing = dispatch_tables(expert_index_table, experts, capacity)
    outgoing = jnp.dot(spread_own, normed, preferred_element_type=jnp.float32).astype(jnp.bfloat16)
    outgoing = outgoing.reshape(experts, capacity, model_width)
    incoming = lax.all_to_all(outgoing, "sp", split_axis=0, concat_axis=0, tiled=True).reshape(
        sp_size * capacity, model_width
    )
    hidden = expand(lax.all_gather(incoming, "tp", axis=0, tiled=True), gate_mat, up_mat)
    summed = lax.psum_scatter(
        jnp.dot(hidden, down_mat, preferred_element_type=jnp.float32).astype(jnp.bfloat16),
        "tp",
        scatter_dimension=0,
        tiled=True,
    )
    returned = lax.all_to_all(
        summed.reshape(sp_size, capacity, model_width),
        "sp",
        split_axis=0,
        concat_axis=0,
        tiled=True,
    )
    pair_out = jnp.einsum(
        "sp,sd->pd",
        routing,
        returned.reshape(experts * capacity, model_width),
        preferred_element_type=jnp.float32,
    ).reshape(row_count, TOPK, model_width)
    weights = jax.nn.sigmoid(expert_router_scores - expert_router_scores[:, ::-1])
    total = mixed_f + jnp.sum(weights[:, :, None] * pair_out, axis=1)
    return total.astype(jnp.bfloat16)


def solution(mesh):
    return jax.shard_map(
        shards,
        mesh=mesh,
        in_specs=(
            P("sp", "tp"),
            P("sp", "tp"),
            P("sp", "tp"),
            P("sp", "tp"),
            P("tp"),
            P("sp", "tp"),
            P("sp", "tp"),
            P("sp", "tp"),
            P("tp"),
            P(),
            P(("sp", "tp"), None),
            P(),
            P(("sp", "tp"), None),
            P(("sp", "tp"), None),
            P("sp", None, "tp"),
            P("sp", None, "tp"),
            P("sp", "tp", None),
        ),
        out_specs=P(("sp", "tp"), None),
        check_vma=False,
    )
```
